32 devices in a mesh: sp: 8 (over z, y), tp: 4 (over x, core).
Axes of the slice: x: 2, y: 2, z: 4, core: 2. Of those that a mesh axis runs over, the one named last changes fastest.
Arguments:
- queries: bfloat16 [3072, 2048], P('sp', 'tp'), may hold values from -200 to 200
- keys: bfloat16 [3072, 2048], P('sp', 'tp'), may hold values from -200 to 200
- values: bfloat16 [3072, 2048], P('sp', 'tp'), may hold values from -6 to 6
- forget_sums: float32 [3072, 16], P('sp', 'tp'), may hold values from -3072 to 0, as said below
- residual_in: bfloat16 [3072, 2048], P(('sp', 'tp')), may hold values from -0.59765625 to 0.59765625
- out_weight: bfloat16 [2048, 2048], P('tp'), may hold values from -0.125 to 0.125
- norm_gain: bfloat16 [2048], replicated, may hold values from 0.099609375 to 1.8984375
- gate_weight: bfloat16 [2048, 3072], P('sp', 'tp'), may hold values from -0.125 to 0.125
- up_weight: bfloat16 [2048, 3072], P('sp', 'tp'), may hold values from -0.125 to 0.125
- down_weight: bfloat16 [3072, 2048], P('tp', 'sp'), may hold values from -0.109375 to 0.109375
Outputs:
- mixed: bfloat16 [3072, 2048], P(('sp', 'tp'))
The draws below stay inside these ranges and needn't reach their ends.
Inputs may be any that keep to these rules, and one draw needn't show every extreme that they name: `forget_sums`: in every head the entries never rise from one position to the next.
All inputs are finite; a program needn't handle non-finite values.
Results may differ from the reference program's by a relative error of at most 0.022.
Values may be sent and summed in bfloat16 or wider, within the bound.
A program may use at most 192 MiB of HBM per device.

```python
import math
import jax
import jax.numpy as jnp
from jax import lax

D = 2048
HEADS = 16
HD = 128
FFW = 3072
TOK_DEV = 384
CONTEXT_LENGTH = 3072
N_TP = 4


def drawn_pair(key):
    starting_shift = jax.random.fold_in(key, 7)
    key_query, key_key = jax.random.split(starting_shift, 2)
    width = HEADS * HD
    queries = jnp.clip(jax.random.normal(key_query, (CONTEXT_LENGTH, width), jnp.float32), -6.0, 6.0)
    keys = jnp.clip(jax.random.normal(key_key, (CONTEXT_LENGTH, width), jnp.float32), -6.0, 6.0)
    return (queries, keys)


def draw_queries(key, part):
    return drawn_pair(key)[0].astype(jnp.bfloat16)


def draw_keys(key, part):
    return drawn_pair(key)[1].astype(jnp.bfloat16)


def draw_forget_sums(key, part):
    starting_shift = jax.random.fold_in(key, 11)
    lookup_arrangement, lookup_panel_group, lookup_spacing, lookup_contiguous_span, lookup_omitted = jax.random.split(starting_shift, 5)
    order = jax.random.permutation(lookup_arrangement, HEADS)
    gradual_attenuation = order < HEADS // 2
    rate = jnp.where(gradual_attenuation, 0.5 / CONTEXT_LENGTH, 1.0 / 40.0).astype(jnp.float32)
    block_count = CONTEXT_LENGTH // TOK_DEV
    block_factor = jnp.exp(jax.random.uniform(lookup_panel_group, (block_count, 1), jnp.float32, jnp.log(0.5), jnp.log(2.0)))
    block_factor = jnp.repeat(block_factor, TOK_DEV, axis=0)
    step_factor = jnp.exp(jax.random.uniform(lookup_spacing, (CONTEXT_LENGTH, HEADS), jnp.float32, jnp.log(0.5), jnp.log(2.0)))
    retention_log_gate = -rate[None, :] * block_factor * step_factor
    contiguous_place = jax.random.randint(lookup_contiguous_span, (3,), 0, CONTEXT_LENGTH)
    omitted_elements = jax.random.uniform(lookup_omitted, (3, HEADS), jnp.float32, jnp.log(0.55), jnp.log(0.8))
    retention_log_gate = retention_log_gate.at[contiguous_place].add(jnp.where(gradual_attenuation[None, :], omitted_elements, 0.0))
    return jnp.cumsum(retention_log_gate, axis=0)


def level_of(key, dims, cuts, smallest, high):
    loudness = 1.0
    for dim, blocks in cuts:
        heights = jax.random.uniform(jax.random.fold_in(jax.random.fold_in(key, 6), dim), (blocks,), jnp.float32, smallest / len(cuts), high / len(cuts))
        loudness = loudness * jnp.repeat(jnp.exp(heights), dims[dim] // blocks).reshape((-1,) + (1,) * (len(dims) - 1 - dim))
    return loudness


def scatter_about(stream_key, shape, scale, limit, cuts=(), kind=jnp.bfloat16):
    result = scale * jax.random.normal(stream_key, shape, jnp.float32)
    if cuts:
        result = result * level_of(stream_key, shape, cuts, -0.22, 0.18)
    return jnp.clip(result, -limit, limit).astype(kind)


def setup_inputs(seed: int = 0) -> dict:
    arg_keys = jax.random.split(jax.random.key(seed), 11)
    queries = draw_queries(jax.random.fold_in(arg_keys[10], 71), 0)
    keys = draw_keys(jax.random.fold_in(arg_keys[10], 71), 0)
    values = scatter_about(arg_keys[2], (CONTEXT_LENGTH, HEADS * HD), 1.0, 6.0, ((0, 8), (1, 4)))
    forget_sums = draw_forget_sums(jax.random.fold_in(arg_keys[10], 71), 0)
    residual_in = scatter_about(arg_keys[4], (CONTEXT_LENGTH, D), 0.1, 0.59765625, ((0, 32),))
    out_weight = scatter_about(arg_keys[5], (HEADS * HD, D), (HEADS * HD) ** -0.5, 0.125, ((0, 4),))
    norm_gain = jnp.clip(1.0 + 0.18 * jax.random.normal(arg_keys[6], (D,), jnp.float32), 0.099609375, 1.8984375).astype(jnp.bfloat16)
    gate_weight = scatter_about(arg_keys[7], (D, FFW), D ** -0.5, 0.125, ((0, 8), (1, 4)))
    up_weight = scatter_about(arg_keys[8], (D, FFW), D ** -0.5, 0.125, ((0, 8), (1, 4)))
    down_weight = scatter_about(arg_keys[9], (FFW, D), FFW ** -0.5, 0.109375, ((0, 4), (1, 8)))
    return {"queries": queries, "keys": keys, "values": values, "forget_sums": forget_sums, "residual_in": residual_in, "out_weight": out_weight, "norm_gain": norm_gain, "gate_weight": gate_weight, "up_weight": up_weight, "down_weight": down_weight}


def attend_head(query_rows, key_rows, value_rows, query_gate):
    block_rows = math.gcd(CONTEXT_LENGTH, 512)
    score_scale = HD ** (-0.5)
    positions = jnp.arange(CONTEXT_LENGTH, dtype=jnp.int32)

    def one_block(start):
        query_block = lax.dynamic_slice_in_dim(query_rows, start, block_rows, 0)
        gate_block = lax.dynamic_slice_in_dim(query_gate, start, block_rows, 0)
        scores = jnp.dot(query_block, key_rows.T, preferred_element_type=jnp.float32) * score_scale
        scores = scores + gate_block[:, None] - query_gate[None, :]
        query_pos = start + jnp.arange(block_rows, dtype=jnp.int32)
        scores = jnp.where(positions[None, :] <= query_pos[:, None], scores, -jnp.inf)
        row_top = lax.optimization_barrier(jnp.max(scores, axis=1, keepdims=True))
        expon = jnp.exp(scores - row_top)
        row_total = lax.optimization_barrier(jnp.sum(expon, axis=1, keepdims=True))
        summed = jnp.dot(expon.astype(jnp.bfloat16), value_rows, preferred_element_type=jnp.float32)
        return (summed / row_total).astype(jnp.bfloat16)
    starts = jnp.arange(CONTEXT_LENGTH // block_rows, dtype=jnp.int32) * block_rows
    return lax.map(one_block, starts).reshape(CONTEXT_LENGTH, HD)

def reference(queries, keys, values, forget_sums, residual_in, out_weight, norm_gain, gate_weight, up_weight, down_weight):
    heads_out = []
    for head_index in range(HEADS):
        columns = slice(head_index * HD, (head_index + 1) * HD)
        heads_out.append(attend_head(queries[:, columns], keys[:, columns], values[:, columns], forget_sums[:, head_index]))
    attended = jnp.concatenate(heads_out, axis=1)
    projected = jnp.dot(attended, out_weight, preferred_element_type=jnp.float32)
    stream = residual_in.astype(jnp.float32) + projected
    normed = stream * lax.rsqrt(lax.optimization_barrier(jnp.mean(stream * stream, axis=1, keepdims=True)) + 1e-06)
    normed = (normed * norm_gain.astype(jnp.float32)).astype(jnp.bfloat16)
    gate = jnp.dot(normed, gate_weight, preferred_element_type=jnp.float32)
    up = jnp.dot(normed, up_weight, preferred_element_type=jnp.float32)
    hidden = (jax.nn.silu(gate) * up).astype(jnp.bfloat16)
    width_part = FFW // N_TP
    summed = jnp.zeros(stream.shape, jnp.float32)
    for index in range(N_TP):
        rows = slice(index * width_part, (index + 1) * width_part)
        partial_value = jnp.dot(hidden[:, rows], down_weight[rows], preferred_element_type=jnp.float32).astype(jnp.bfloat16)
        partial_value = lax.optimization_barrier(partial_value)
        summed = summed + partial_value.astype(jnp.float32)
    return (stream + summed).astype(jnp.bfloat16)
```

```python
import functools
import math

import jax
import jax.numpy as jnp
from jax import lax
from jax.experimental import pallas as pl
from jax.experimental.pallas import tpu as pltpu
from jax.sharding import PartitionSpec as P

HD = 128
F32 = jnp.float32
BF16 = jnp.bfloat16


def remote(src, dst, send_sem, recv_sem, **where):
    return pltpu.make_async_remote_copy(
        src_ref=src,
        dst_ref=dst,
        send_sem=send_sem,
        recv_sem=recv_sem,
        device_id=where,
        device_id_type=pl.DeviceIdType.MESH,
    )


def layer_kernel(
    n, n_tp, heads,
    q, k, v, ft, res, ow, gain, gw, uw, dw,
    out,
    qb, kb, vb, fb, ob, ab, pb, rb, st, xb, gb, ub, db, hb, p2, r2,
    local_sem, qs, qr, fs, fr, kzs, kys, kr, vzs, vys, vr,
    wus, wds, wys, wr, os_, or_, ps, pr, xs, xr, es, er,
):
    sp, tp = lax.axis_index("sp"), lax.axis_index("tp")
    n_z = heads
    n_y = n // n_z
    z, y = sp // n_y, lax.rem(sp, n_y)
    rows = q.shape[0]
    q_rows = rows // n_y
    t_rows = rows // n_tp
    width = ow.shape[1]
    up_depth = gw.shape[0]

    def head_cols(head):
        return pl.ds(pl.multiple_of(head * HD, HD), HD)

    def stripe(part):
        return pl.ds(pl.multiple_of(part * q_rows, q_rows), q_rows)

    def tp_rows(part):
        return pl.ds(pl.multiple_of(part * t_rows, t_rows), t_rows)

    sends = []

    def go(copy):
        copy.start()
        sends.append(copy)

    own = [
        (k.at[:, head_cols(z)], kb.at[sp]),
        (v.at[:, head_cols(z)], vb.at[sp]),
        (q.at[stripe(y), head_cols(z)], qb.at[sp]),
        (ft, fb.at[sp]),
        (gw, gb.at[pl.ds(pl.multiple_of(sp * up_depth, up_depth), up_depth)]),
        (uw, ub.at[pl.ds(pl.multiple_of(sp * up_depth, up_depth), up_depth)]),
        (dw, db.at[sp]),
    ]
    own = [pltpu.make_async_copy(a, b, local_sem.at[i]) for i, (a, b) in enumerate(own)]
    for copy in own:
        copy.start()
    for off in range(1, n_z):
        dz = lax.rem(z + off, n_z)
        for src, buf, ss, rs in ((k, kb, kzs, kr), (v, vb, vzs, vr)):
            go(remote(src.at[:, head_cols(dz)], buf.at[sp], ss.at[dz], rs.at[sp], sp=dz * n_y + y))
    for off in range(1, n):
        d = lax.rem(sp + off, n)
        dz, dy = d // n_y, lax.rem(d, n_y)
        go(remote(q.at[stripe(dy), head_cols(dz)], qb.at[sp], qs.at[d], qr.at[sp], sp=d))
        go(remote(ft, fb.at[sp], fs.at[d], fr.at[sp], sp=d))

    def weight_slot(item, j):
        if item == 2:
            return db.at[j]
        return (gb, ub)[item].at[pl.ds(pl.multiple_of(j * up_depth, up_depth), up_depth)]

    def weight_up(item, j, d):
        return remote(weight_slot(item, j), weight_slot(item, j), wus.at[item, d], wr.at[item, j], sp=sp + n_y)

    def weight_down(item, j, d):
        return remote(weight_slot(item, j), weight_slot(item, j), wds.at[item, d], wr.at[item, j], sp=sp - n_y)

    def weight_side(item, j, d, oy):
        peer = z * n_y + lax.rem(y + oy, n_y)
        return remote(weight_slot(item, j), weight_slot(item, j), wys.at[item, d, oy], wr.at[item, j], sp=peer)

    def weight_came(item, j):
        weight_up(item, j, 0).wait_recv()

    def pass_on(item, d, act):
        @pl.when(z >= d)
        def _():
            j = sp - d * n_y
            if act == "start":
                weight_came(item, j)

            @pl.when(z < n_z - 1)
            def _():
                getattr(weight_up(item, j, d), act)()

            for oy in range(1, n_y):
                getattr(weight_side(item, j, d, oy), act)()

        @pl.when(z + d < n_z)
        def _():
            j = sp + d * n_y
            if act == "start":
                weight_came(item, j)

            @pl.when(z > 0)
            def _():
                getattr(weight_down(item, j, d), act)()

            for oy in range(1, n_y):
                getattr(weight_side(item, j, n_z - 1 + d, oy), act)()

    def own_lines(item, act):
        @pl.when(z < n_z - 1)
        def _():
            getattr(weight_up(item, sp, 0), act)()

        @pl.when(z > 0)
        def _():
            getattr(weight_down(item, sp, 0), act)()

    def own_sides(item, act):
        for oy in range(1, n_y):
            getattr(weight_side(item, sp, 0, oy), act)()

    for copy in own[4:]:
        copy.wait()
    for item in range(3):
        own_lines(item, "start")

    for copy in own[:4]:
        copy.wait()
    for off in range(n_z):
        src = lax.rem(z + off, n_z) * n_y + y
        for buf, ss, rs in ((kb, kys, kr), (vb, vys, vr)):
            if off:
                remote(buf.at[src], buf.at[src], ss.at[off, 0], rs.at[src], sp=sp).wait_recv()
            for oy in range(1, n_y):
                peer = z * n_y + lax.rem(y + oy, n_y)
                go(remote(buf.at[src], buf.at[src], ss.at[off, oy], rs.at[src], sp=peer))
    for item in range(3):
        own_sides(item, "start")
    for oy in range(1, n_y):
        for zz in range(n_z):
            src = zz * n_y + lax.rem(y + oy, n_y)
            for buf, ss, rs in ((kb, kys, kr), (vb, vys, vr)):
                remote(buf.at[src], buf.at[src], ss.at[0, 0], rs.at[src], sp=sp).wait_recv()
    for off in range(1, n):
        src = lax.rem(sp + off, n)
        remote(qb.at[src], qb.at[src], qs.at[src], qr.at[src], sp=sp).wait_recv()
        remote(fb.at[src], fb.at[src], fs.at[src], fr.at[src], sp=sp).wait_recv()

    pass_on(0, 1, "start")

    head_pick = lax.broadcasted_iota(jnp.int32, fb.shape[1:], 0) == z
    row_id = lax.broadcasted_iota(jnp.int32, (q_rows, rows), 0) + y * q_rows
    col_id = lax.broadcasted_iota(jnp.int32, (q_rows, rows), 1)

    def gate_row(j):
        return jnp.sum(jnp.where(head_pick, fb[j], 0.0), axis=0, keepdims=True)

    def attend(i, unused):
        query = qb[i]
        query_gate = jnp.sum(jnp.where(row_id == col_id, gate_row(i), 0.0), axis=1, keepdims=True)

        def block(j, carried):
            top, total, weighted = carried
            scores = lax.dot_general(
                query, kb[j], (((1,), (1,)), ((), ())), preferred_element_type=F32
            ) * (HD ** -0.5)
            scores = scores + query_gate - gate_row(j)
            scores = jnp.where(col_id + (j - i) * rows <= row_id, scores, -jnp.inf)
            new_top = jnp.maximum(top, jnp.max(scores, axis=1, keepdims=True))
            shrink = jnp.exp(top - new_top)
            expon = jnp.exp(scores - new_top)
            total = shrink * total + jnp.sum(expon, axis=1, keepdims=True)
            weighted = shrink * weighted + jnp.dot(expon.astype(BF16), vb[j], preferred_element_type=F32)
            return new_top, total, weighted

        start = (
            jnp.full((q_rows, 1), -1e30, F32),
            jnp.zeros((q_rows, 1), F32),
            jnp.zeros((q_rows, HD), F32),
        )
        top, total, weighted = lax.fori_loop(0, i + 1, block, start)
        ob[i] = (weighted / total).astype(BF16)
        return unused

    lax.fori_loop(0, n, attend, 0)

    back = pltpu.make_async_copy(ob.at[sp], ab.at[stripe(y), head_cols(z)], local_sem.at[0])
    back.start()
    for off in range(1, n):
        d = lax.rem(sp + off, n)
        go(remote(ob.at[d], ab.at[stripe(y), head_cols(z)], os_.at[d], or_.at[sp], sp=d))
    pass_on(1, 1, "start")
    pass_on(2, 1, "start")
    back.wait()
    for off in range(1, n):
        src = lax.rem(sp + off, n)
        slot = ab.at[stripe(lax.rem(src, n_y)), head_cols(src // n_y)]
        remote(slot, slot, os_.at[src], or_.at[src], sp=sp).wait_recv()

    tile = math.gcd(width, 256)

    def project(c, unused):
        cols = pl.ds(pl.multiple_of(c * tile, tile), tile)
        pb[:, cols] = jnp.dot(ab[...], ow[:, cols], preferred_element_type=F32).astype(BF16)
        return unused

    lax.fori_loop(0, width // tile, project, 0)
    peers = [lax.rem(tp + off, n_tp) for off in range(1, n_tp)]
    for t in peers:
        go(remote(pb.at[tp_rows(t)], rb.at[tp], ps.at[t], pr.at[tp], tp=t))
    pass_on(0, 2, "start")
    for t in peers:
        remote(rb.at[t], rb.at[t], ps.at[t], pr.at[t], tp=tp).wait_recv()
    step = math.gcd(t_rows, 16)

    def normalise(r, unused):
        here = pl.ds(pl.multiple_of(r * step, step), step)
        there = pl.ds(pl.multiple_of(tp * t_rows + r * step, step), step)
        total = pb[there].astype(F32)
        for t in peers:
            total = total + rb[t, here].astype(F32)
        stream = res[here].astype(F32) + total
        st[here] = stream
        mean = jnp.mean(stream * stream, axis=1, keepdims=True)
        xb[there] = (stream * lax.rsqrt(mean + 1e-06) * gain[...].astype(F32)).astype(BF16)
        return unused

    lax.fori_loop(0, t_rows // step, normalise, 0)
    for t in peers:
        go(remote(xb.at[tp_rows(tp)], xb.at[tp_rows(tp)], xs.at[t], xr.at[tp], tp=t))
    pass_on(1, 2, "start")
    pass_on(2, 2, "start")
    for d in range(3, n_z):
        for item in range(3):
            pass_on(item, d, "start")
    for t in peers:
        remote(xb.at[tp_rows(t)], xb.at[tp_rows(t)], xs.at[t], xr.at[t], tp=tp).wait_recv()

    def sides_came(item):
        for zz in range(n_z):
            for oy in range(1, n_y):
                weight_came(item, zz * n_y + lax.rem(y + oy, n_y))

    sides_came(0)
    sides_came(1)
    ffw = gw.shape[1]
    ftile = math.gcd(ffw, 256)

    def widen(c, unused):
        cols = pl.ds(pl.multiple_of(c * ftile, ftile), ftile)
        gate = jnp.dot(xb[...], gb[:, cols], preferred_element_type=F32)
        up = jnp.dot(xb[...], ub[:, cols], preferred_element_type=F32)
        hb[:, cols] = (gate / (1.0 + jnp.exp(-gate)) * up).astype(BF16)
        return unused

    lax.fori_loop(0, ffw // ftile, widen, 0)
    sides_came(2)
    d_cols = dw.shape[1]
    group = max(1, 128 // d_cols)

    def narrow(c, unused):
        parts = [jnp.dot(hb[...], db[c * group + g], preferred_element_type=F32) for g in range(group)]
        joined = parts[0] if group == 1 else jnp.concatenate(parts, axis=1)
        p2[:, pl.ds(pl.multiple_of(c * group * d_cols, group * d_cols), group * d_cols)] = joined.astype(BF16)
        return unused

    lax.fori_loop(0, n // group, narrow, 0)
    for t in peers:
        go(remote(p2.at[tp_rows(t)], r2.at[tp], es.at[t], er.at[tp], tp=t))
    for t in peers:
        remote(r2.at[t], r2.at[t], es.at[t], er.at[t], tp=tp).wait_recv()

    def finish(r, unused):
        here = pl.ds(pl.multiple_of(r * step, step), step)
        there = pl.ds(pl.multiple_of(tp * t_rows + r * step, step), step)
        total = p2[there].astype(F32)
        for t in peers:
            total = total + r2[t, here].astype(F32)
        out[here] = (st[here] + total).astype(BF16)
        return unused

    lax.fori_loop(0, t_rows // step, finish, 0)

    for copy in sends:
        copy.wait_send()
    for item in range(3):
        own_lines(item, "wait_send")
        own_sides(item, "wait_send")
        for d in range(1, n_z):
            pass_on(item, d, "wait_send")


def shards(n, n_tp, q, k, v, forget_sums, residual_in, out_weight, norm_gain, gate_weight, up_weight, down_weight):
    rows, wide = q.shape
    heads = wide // HD
    n_y = n // heads
    q_rows, t_rows, width = rows // n_y, rows // n_tp, out_weight.shape[1]
    ffw, d_cols = gate_weight.shape[1], down_weight.shape[1]
    lanes = -(-heads // 8) * 8
    ft = jnp.pad(forget_sums.T, ((0, lanes - heads), (0, 0)))
    dma = lambda *shape: pltpu.SemaphoreType.DMA(shape)
    scratch = [
        pltpu.VMEM((n, q_rows, HD), BF16),
        pltpu.VMEM((n, rows, HD), BF16),
        pltpu.VMEM((n, rows, HD), BF16),
        pltpu.VMEM((n, lanes, rows), F32),
        pltpu.VMEM((n, q_rows, HD), BF16),
        pltpu.VMEM((rows, wide), BF16),
        pltpu.VMEM((rows, width), BF16),
        pltpu.VMEM((n_tp, t_rows, width), BF16),
        pltpu.VMEM((t_rows, width), F32),
        pltpu.VMEM((rows, width), BF16),
        pltpu.VMEM((width, ffw), BF16),
        pltpu.VMEM((width, ffw), BF16),
        pltpu.VMEM((n, ffw, d_cols), BF16),
        pltpu.VMEM((rows, ffw), BF16),
        pltpu.VMEM((rows, width), BF16),
        pltpu.VMEM((n_tp, t_rows, width), BF16),
        dma(7), dma(n), dma(n), dma(n), dma(n),
        dma(heads), dma(heads, n_y), dma(n), dma(heads), dma(heads, n_y), dma(n),
        dma(3, heads), dma(3, heads), dma(3, 2 * heads, n_y), dma(3, n),
        dma(n), dma(n), dma(n_tp), dma(n_tp), dma(n_tp), dma(n_tp), dma(n_tp), dma(n_tp),
    ]
    vmem = pl.BlockSpec(memory_space=pltpu.VMEM)
    return pl.pallas_call(
        functools.partial(layer_kernel, n, n_tp, heads),
        out_shape=jax.ShapeDtypeStruct((t_rows, width), BF16),
        in_specs=[vmem] * 10,
        out_specs=vmem,
        scratch_shapes=scratch,
        compiler_params=pltpu.CompilerParams(has_side_effects=True, vmem_limit_bytes=60 * 1024 * 1024),
    )(q, k, v, ft, residual_in, out_weight, norm_gain.reshape(1, -1), gate_weight, up_weight, down_weight)


def solution(mesh):
    placed = (
        P("sp", "tp"),
        P("sp", "tp"),
        P("sp", "tp"),
        P("sp", "tp"),
        P(("sp", "tp"), None),
        P("tp", None),
        P(),
        P("sp", "tp"),
        P("sp", "tp"),
        P("tp", "sp"),
    )
    return jax.shard_map(
        functools.partial(shards, mesh.shape["sp"], mesh.shape["tp"]),
        mesh=mesh, in_specs=placed, out_specs=P(("sp", "tp"), None), check_vma=False,
    )
```

```python
import functools
import math

import jax
import jax.numpy as jnp
from jax import lax
from jax.experimental import pallas as pl
from jax.experimental.pallas import tpu as pltpu
from jax.sharding import PartitionSpec as P

HD = 128
F32 = jnp.float32
BF16 = jnp.bfloat16


def remote(src, dst, send_sem, recv_sem, **where):
    return pltpu.make_async_remote_copy(
        src_ref=src,
        dst_ref=dst,
        send_sem=send_sem,
        recv_sem=recv_sem,
        device_id=where,
        device_id_type=pl.DeviceIdType.MESH,
    )


def layer_kernel(
    n, n_tp, heads,
    q, k, v, ft, res, ow, gain, gw, uw, dw,
    out,
    qb, kb, vb, fb, ob, ab, pb, s1, s2, st, xb, gb, ub, db, hb, p2, e1, e2,
    local_sem, qs, qr, fs, fr, kzs, kys, kr, vzs, vys, vr,
    wus, wds, wys, wr, aus, ads, ays, ar, os_, or_, ps, pr, p2s, p2r, xs, xr, xf, es, er, e2s, e2r,
):
    sp, tp = lax.axis_index("sp"), lax.axis_index("tp")
    n_z = heads
    n_y = n // n_z
    z, y = sp // n_y, lax.rem(sp, n_y)
    rows = q.shape[0]
    q_rows = rows // n_y
    t_rows = rows // n_tp
    width = ow.shape[1]
    up_depth = gw.shape[0]

    def head_cols(head):
        return pl.ds(pl.multiple_of(head * HD, HD), HD)

    def stripe(part):
        return pl.ds(pl.multiple_of(part * q_rows, q_rows), q_rows)

    def tp_rows(part):
        return pl.ds(pl.multiple_of(part * t_rows, t_rows), t_rows)

    sends = []

    def go(copy):
        copy.start()
        sends.append(copy)

    own = [
        (k.at[:, head_cols(z)], kb.at[sp]),
        (v.at[:, head_cols(z)], vb.at[sp]),
        (q.at[stripe(y), head_cols(z)], qb.at[sp]),
        (ft, fb.at[sp]),
        (gw, gb.at[pl.ds(pl.multiple_of(sp * up_depth, up_depth), up_depth)]),
        (uw, ub.at[pl.ds(pl.multiple_of(sp * up_depth, up_depth), up_depth)]),
        (dw, db.at[sp]),
    ]
    own = [pltpu.make_async_copy(a, b, local_sem.at[i]) for i, (a, b) in enumerate(own)]
    for copy in own:
        copy.start()
    for off in range(1, n_z):
        dz = lax.rem(z + off, n_z)
        for src, buf, ss, rs in ((k, kb, kzs, kr), (v, vb, vzs, vr)):
            go(remote(src.at[:, head_cols(dz)], buf.at[sp], ss.at[dz], rs.at[sp], sp=dz * n_y + y))
    for off in range(1, n):
        d = lax.rem(sp + off, n)
        dz, dy = d // n_y, lax.rem(d, n_y)
        go(remote(q.at[stripe(dy), head_cols(dz)], qb.at[sp], qs.at[d], qr.at[sp], sp=d))
        go(remote(ft, fb.at[sp], fs.at[d], fr.at[sp], sp=d))

    half = dw.shape[0] // 2

    def weight_slot(item, j):
        if item == 2:
            return db.at[j, :half]
        return (gb, ub)[item].at[pl.ds(pl.multiple_of(j * up_depth, up_depth), up_depth)]

    def weight_up(item, j, d):
        return remote(weight_slot(item, j), weight_slot(item, j), wus.at[item, d], wr.at[item, j], sp=sp + n_y)

    def weight_down(item, j, d):
        return remote(weight_slot(item, j), weight_slot(item, j), wds.at[item, d], wr.at[item, j], sp=sp - n_y)

    def weight_side(item, j, d, oy):
        peer = z * n_y + lax.rem(y + oy, n_y)
        return remote(weight_slot(item, j), weight_slot(item, j), wys.at[item, d, oy], wr.at[item, j], sp=peer)

    def weight_came(item, j):
        weight_up(item, j, 0).wait_recv()

    def pass_on(item, d, act):
        @pl.when(z >= d)
        def _():
            j = sp - d * n_y
            if act == "start":
                weight_came(item, j)

            @pl.when(z < n_z - 1)
            def _():
                getattr(weight_up(item, j, d), act)()

            for oy in range(1, n_y):
                getattr(weight_side(item, j, d, oy), act)()

        @pl.when(z + d < n_z)
        def _():
            j = sp + d * n_y
            if act == "start":
                weight_came(item, j)

            @pl.when(z > 0)
            def _():
                getattr(weight_down(item, j, d), act)()

            for oy in range(1, n_y):
                getattr(weight_side(item, j, n_z - 1 + d, oy), act)()

    def own_lines(item, act):
        @pl.when(z < n_z - 1)
        def _():
            getattr(weight_up(item, sp, 0), act)()

        @pl.when(z > 0)
        def _():
            getattr(weight_down(item, sp, 0), act)()

    def own_sides(item, act):
        for oy in range(1, n_y):
            getattr(weight_side(item, sp, 0, oy), act)()

    def late_copy(j, send_sem, peer):
        return remote(db.at[j, half:], db.at[j, half:], send_sem, ar.at[j], sp=peer)

    def late_came(j):
        late_copy(j, aus.at[0, 0], sp).wait_recv()

    def late_sides(act):
        for oy in range(1, n_y):
            getattr(late_copy(sp, ays.at[oy], z * n_y + lax.rem(y + oy, n_y)), act)()

    def late_lines(d, act):
        for oy in range(n_y):
            column = lax.rem(y + oy, n_y)

            below, above = (z - d) * n_y + column, (z + d) * n_y + column
            if act == "start" and (d or oy):
                @pl.when(z >= d)
                def _():
                    late_came(below)

            if act == "start" and d:
                @pl.when(z + d < n_z)
                def _():
                    late_came(above)

            if d < n_z - 1:
                @pl.when(jnp.minimum(z - d, n_z - 2 - z) >= 0)
                def _():
                    getattr(late_copy(below, aus.at[d, oy], sp + n_y), act)()

                @pl.when(jnp.minimum(z - 1, n_z - 1 - d - z) >= 0)
                def _():
                    getattr(late_copy(above, ads.at[d, oy], sp - n_y), act)()

    for copy in own[4:]:
        copy.wait()
    for item in range(3):
        own_lines(item, "start")

    for copy in own[:4]:
        copy.wait()
    for off in range(n_z):
        src = lax.rem(z + off, n_z) * n_y + y
        for buf, ss, rs in ((kb, kys, kr), (vb, vys, vr)):
            if off:
                remote(buf.at[src], buf.at[src], ss.at[off, 0], rs.at[src], sp=sp).wait_recv()
            for oy in range(1, n_y):
                peer = z * n_y + lax.rem(y + oy, n_y)
                go(remote(buf.at[src], buf.at[src], ss.at[off, oy], rs.at[src], sp=peer))
    late_sides("start")
    for item in range(3):
        own_sides(item, "start")
    for oy in range(1, n_y):
        for zz in range(n_z):
            src = zz * n_y + lax.rem(y + oy, n_y)
            for buf, ss, rs in ((kb, kys, kr), (vb, vys, vr)):
                remote(buf.at[src], buf.at[src], ss.at[0, 0], rs.at[src], sp=sp).wait_recv()
    for off in range(1, n):
        src = lax.rem(sp + off, n)
        remote(qb.at[src], qb.at[src], qs.at[src], qr.at[src], sp=sp).wait_recv()
        remote(fb.at[src], fb.at[src], fs.at[src], fr.at[src], sp=sp).wait_recv()

    head_pick = lax.broadcasted_iota(jnp.int32, fb.shape[1:], 0) == z
    row_id = lax.broadcasted_iota(jnp.int32, (q_rows, rows), 0) + y * q_rows
    col_id = lax.broadcasted_iota(jnp.int32, (q_rows, rows), 1)

    def gate_row(j):
        return jnp.sum(jnp.where(head_pick, fb[j], 0.0), axis=0, keepdims=True)

    def attend(i, unused):
        query = qb[i]
        query_gate = jnp.sum(jnp.where(row_id == col_id, gate_row(i), 0.0), axis=1, keepdims=True)

        def block(j, carried):
            top, total, weighted = carried
            scores = lax.dot_general(
                query, kb[j], (((1,), (1,)), ((), ())), preferred_element_type=F32
            ) * (HD ** -0.5)
            scores = scores + query_gate - gate_row(j)
            scores = jnp.where(col_id + (j - i) * rows <= row_id, scores, -jnp.inf)
            new_top = jnp.maximum(top, jnp.max(scores, axis=1, keepdims=True))
            shrink = jnp.exp(top - new_top)
            expon = jnp.exp(scores - new_top)
            total = shrink * total + jnp.sum(expon, axis=1, keepdims=True)
            weighted = shrink * weighted + jnp.dot(expon.astype(BF16), vb[j], preferred_element_type=F32)
            return new_top, total, weighted

        start = (
            jnp.full((q_rows, 1), -1e30, F32),
            jnp.zeros((q_rows, 1), F32),
            jnp.zeros((q_rows, HD), F32),
        )
        top, total, weighted = lax.fori_loop(0, i + 1, block, start)
        ob[i] = (weighted / total).astype(BF16)
        return unused

    lax.fori_loop(0, n, attend, 0)

    back = pltpu.make_async_copy(ob.at[sp], ab.at[stripe(y), head_cols(z)], local_sem.at[0])
    back.start()
    for off in range(1, n):
        d = lax.rem(sp + off, n)
        go(remote(ob.at[d], ab.at[stripe(y), head_cols(z)], os_.at[d], or_.at[sp], sp=d))
    for item in range(3):
        pass_on(item, 1, "start")
    back.wait()
    for off in range(1, n):
        src = lax.rem(sp + off, n)
        slot = ab.at[stripe(lax.rem(src, n_y)), head_cols(src // n_y)]
        remote(slot, slot, os_.at[src], or_.at[src], sp=sp).wait_recv()

    tile = math.gcd(width, 256)

    def project(c, unused):
        cols = pl.ds(pl.multiple_of(c * tile, tile), tile)
        pb[:, cols] = jnp.dot(ab[...], ow[:, cols], preferred_element_type=F32).astype(BF16)
        return unused

    lax.fori_loop(0, width // tile, project, 0)
    n_c = 2 if n_tp % 2 == 0 else 1
    n_a = n_tp // n_c
    a_here, c_here = tp // n_c, lax.rem(tp, n_c)
    a_peers = [lax.rem(a_here + off, n_a) for off in range(1, n_a)]
    c_peers = [lax.rem(c_here + off, n_c) for off in range(1, n_c)]
    step = math.gcd(t_rows, 16)

    def near_sends(part, near, ss, rs):
        for a in a_peers + [a_here]:
            for c in c_peers:
                go(remote(part.at[tp_rows(a * n_c + c)], near.at[c_here, a], ss.at[a, c], rs.at[c_here, a],
                          tp=a_here * n_c + c))

    def near_wait(near, a, ss, rs):
        for c in c_peers:
            remote(near.at[c, a], near.at[c, a], ss.at[a, c], rs.at[c, a], tp=tp).wait_recv()

    def far_sends(part, near, far, ss, rs, far_ss, far_rs):
        for a in a_peers:
            near_wait(near, a, ss, rs)

            def add(r, unused, a=a):
                here = pl.ds(pl.multiple_of(r * step, step), step)
                there = pl.ds(pl.multiple_of((a * n_c + c_here) * t_rows + r * step, step), step)
                total = part[there].astype(F32)
                for c in c_peers:
                    total = total + near[c, a, here].astype(F32)
                part[there] = total.astype(BF16)
                return unused

            lax.fori_loop(0, t_rows // step, add, 0)
        for a in a_peers:
            go(remote(part.at[tp_rows(a * n_c + c_here)], far.at[a_here], far_ss.at[a], far_rs.at[a_here],
                      tp=a * n_c + c_here))

    def far_wait(near, far, ss, rs, far_ss, far_rs):
        near_wait(near, a_here, ss, rs)
        for a in a_peers:
            remote(far.at[a], far.at[a], far_ss.at[a], far_rs.at[a], tp=tp).wait_recv()

    def summed(part, near, far, here, there):
        total = part[there].astype(F32)
        for c in c_peers:
            total = total + near[c, a_here, here].astype(F32)
        for a in a_peers:
            total = total + far[a, here].astype(F32)
        return total

    near_sends(pb, s1, ps, pr)
    far_sends(pb, s1, s2, ps, pr, p2s, p2r)
    for item in range(3):
        pass_on(item, 2, "start")
    late_lines(0, "start")
    far_wait(s1, s2, ps, pr, p2s, p2r)

    def normalise(r, unused):
        here = pl.ds(pl.multiple_of(r * step, step), step)
        there = pl.ds(pl.multiple_of(tp * t_rows + r * step, step), step)
        stream = res[here].astype(F32) + summed(pb, s1, s2, here, there)
        st[here] = stream
        mean = jnp.mean(stream * stream, axis=1, keepdims=True)
        xb[there] = (stream * lax.rsqrt(mean + 1e-06) * gain[...].astype(F32)).astype(BF16)
        return unused

    lax.fori_loop(0, t_rows // step, normalise, 0)
    def rows_to(t_src, t_dst, ss):
        return remote(xb.at[tp_rows(t_src)], xb.at[tp_rows(t_src)], ss, xr.at[t_src], tp=t_dst)

    for a in a_peers:
        go(rows_to(tp, a * n_c + c_here, xs.at[a * n_c + c_here]))
    for c in c_peers:
        go(rows_to(tp, a_here * n_c + c, xs.at[a_here * n_c + c]))
    if n_z > 3:
        pass_on(0, 3, "start")
    for a in a_peers:
        t = a * n_c + c_here
        rows_to(t, tp, xs.at[t]).wait_recv()
        for c in c_peers:
            go(rows_to(t, a_here * n_c + c, xf.at[a, c]))
    for d in range(3, n_z):
        for item in range(3):
            if (item, d) != (0, 3):
                if item == 2 and d == 3:
                    late_lines(1, "start")
                pass_on(item, d, "start")
    if n_z <= 3:
        late_lines(1, "start")
    for d in range(2, n_z):
        if d < n_z - 1:
            late_lines(d, "start")
    for a in range(n_a):
        for c in c_peers:
            t = a * n_c + c
            rows_to(t, tp, xs.at[t]).wait_recv()

    def sides_came(item):
        for zz in range(n_z):
            for oy in range(1, n_y):
                weight_came(item, zz * n_y + lax.rem(y + oy, n_y))

    sides_came(0)
    sides_came(1)
    ffw = gw.shape[1]
    ftile = math.gcd(ffw, 256)

    def widen(c, unused):
        cols = pl.ds(pl.multiple_of(c * ftile, ftile), ftile)
        gate = jnp.dot(xb[...], gb[:, cols], preferred_element_type=F32)
        up = jnp.dot(xb[...], ub[:, cols], preferred_element_type=F32)
        hb[:, cols] = (gate / (1.0 + jnp.exp(-gate)) * up).astype(BF16)
        return unused

    lax.fori_loop(0, ffw // ftile, widen, 0)
    sides_came(2)
    late_lines(n_z - 1, "start")
    d_cols = dw.shape[1]
    group = max(1, 128 // d_cols)

    def narrow(c, unused):
        parts = [jnp.dot(hb[...], db[c * group + g], preferred_element_type=F32) for g in range(group)]
        joined = parts[0] if group == 1 else jnp.concatenate(parts, axis=1)
        p2[:, pl.ds(pl.multiple_of(c * group * d_cols, group * d_cols), group * d_cols)] = joined.astype(BF16)
        return unused

    lax.fori_loop(0, n // group, narrow, 0)
    near_sends(p2, e1, es, er)
    far_sends(p2, e1, e2, es, er, e2s, e2r)
    far_wait(e1, e2, es, er, e2s, e2r)

    def finish(r, unused):
        here = pl.ds(pl.multiple_of(r * step, step), step)
        there = pl.ds(pl.multiple_of(tp * t_rows + r * step, step), step)
        out[here] = (st[here] + summed(p2, e1, e2, here, there)).astype(BF16)
        return unused

    lax.fori_loop(0, t_rows // step, finish, 0)

    for copy in sends:
        copy.wait_send()
    for item in range(3):
        own_lines(item, "wait_send")
        own_sides(item, "wait_send")
        for d in range(1, n_z):
            pass_on(item, d, "wait_send")
    late_sides("wait_send")
    for d in range(n_z):
        late_lines(d, "wait_send")


def shards(n, n_tp, q, k, v, forget_sums, residual_in, out_weight, norm_gain, gate_weight, up_weight, down_weight):
    rows, wide = q.shape
    heads = wide // HD
    n_y = n // heads
    q_rows, t_rows, width = rows // n_y, rows // n_tp, out_weight.shape[1]
    ffw, d_cols = gate_weight.shape[1], down_weight.shape[1]
    n_c = 2 if n_tp % 2 == 0 else 1
    n_a = n_tp // n_c
    lanes = -(-heads // 8) * 8
    ft = jnp.pad(forget_sums.T, ((0, lanes - heads), (0, 0)))
    dma = lambda *shape: pltpu.SemaphoreType.DMA(shape)
    scratch = [
        pltpu.VMEM((n, q_rows, HD), BF16),
        pltpu.VMEM((n, rows, HD), BF16),
        pltpu.VMEM((n, rows, HD), BF16),
        pltpu.VMEM((n, lanes, rows), F32),
        pltpu.VMEM((n, q_rows, HD), BF16),
        pltpu.VMEM((rows, wide), BF16),
        pltpu.VMEM((rows, width), BF16),
        pltpu.VMEM((n_c, n_a, t_rows, width), BF16),
        pltpu.VMEM((n_a, t_rows, width), BF16),
        pltpu.VMEM((t_rows, width), F32),
        pltpu.VMEM((rows, width), BF16),
        pltpu.VMEM((width, ffw), BF16),
        pltpu.VMEM((width, ffw), BF16),
        pltpu.VMEM((n, ffw, d_cols), BF16),
        pltpu.VMEM((rows, ffw), BF16),
        pltpu.VMEM((rows, width), BF16),
        pltpu.VMEM((n_c, n_a, t_rows, width), BF16),
        pltpu.VMEM((n_a, t_rows, width), BF16),
        dma(7), dma(n), dma(n), dma(n), dma(n),
        dma(heads), dma(heads, n_y), dma(n), dma(heads), dma(heads, n_y), dma(n),
        dma(3, heads), dma(3, heads), dma(3, 2 * heads, n_y), dma(3, n),
        dma(heads, n_y), dma(heads, n_y), dma(n_y), dma(n),
        dma(n), dma(n), dma(n_a, n_c), dma(n_c, n_a), dma(n_a), dma(n_a),
        dma(n_tp), dma(n_tp), dma(n_a, n_c), dma(n_a, n_c), dma(n_c, n_a), dma(n_a), dma(n_a),
    ]
    vmem = pl.BlockSpec(memory_space=pltpu.VMEM)
    return pl.pallas_call(
        functools.partial(layer_kernel, n, n_tp, heads),
        out_shape=jax.ShapeDtypeStruct((t_rows, width), BF16),
        in_specs=[vmem] * 10,
        out_specs=vmem,
        scratch_shapes=scratch,
        compiler_params=pltpu.CompilerParams(has_side_effects=True, vmem_limit_bytes=60 * 1024 * 1024),
    )(q, k, v, ft, residual_in, out_weight, norm_gain.reshape(1, -1), gate_weight, up_weight, down_weight)


def solution(mesh):
    placed = (
        P("sp", "tp"),
        P("sp", "tp"),
        P("sp", "tp"),
        P("sp", "tp"),
        P(("sp", "tp"), None),
        P("tp", None),
        P(),
        P("sp", "tp"),
        P("sp", "tp"),
        P("tp", "sp"),
    )
    return jax.shard_map(
        functools.partial(shards, mesh.shape["sp"], mesh.shape["tp"]),
        mesh=mesh, in_specs=placed, out_specs=P(("sp", "tp"), None), check_vma=False,
    )
```
